256 devices in a mesh: kv: 32 (over z, y), tp: 8 (over x, core).
Axes of the slice: x: 4, y: 4, z: 8, core: 2. Of those that a mesh axis runs over, the one named last changes fastest.
Arguments:
- tokens: bfloat16 [128, 4096], P(None, ('kv', 'tp')), may hold values from -12 to 12
- first_gain: bfloat16 [4096], replicated, may hold values from 0.099609375 to 1.8984375
- first_gate: bfloat16 [4096, 11264], P(None, ('kv', 'tp')), may hold values from -0.09375 to 0.09375
- first_up: bfloat16 [4096, 11264], P(None, ('kv', 'tp')), may hold values from -0.09375 to 0.09375
- first_down: bfloat16 [11264, 4096], P(('kv', 'tp')), may hold values from -0.25 to 0.25
- mix_gain: bfloat16 [4096], replicated, may hold values from 0.099609375 to 1.8984375
- query_weight: bfloat16 [4096, 1024], P('kv', 'tp'), may hold values from -0.09375 to 0.09375
- key_weight: bfloat16 [4096, 1024], P('kv', 'tp'), may hold values from -0.09375 to 0.09375
- value_weight: bfloat16 [4096, 2048], P('kv', 'tp'), may hold values from -0.09375 to 0.09375
- outgate_weight: bfloat16 [4096, 2048], P('kv', 'tp'), may hold values from -0.09375 to 0.09375
- ingate_weight: bfloat16 [4096, 8], P('kv'), may hold values from -0.09375 to 0.09375
- forget_weight: bfloat16 [4096, 8], P('kv'), may hold values from -0.09375 to 0.09375
- forget_bias: float32 [8], P('tp'), may hold values from -1 to 4
- head_gain: bfloat16 [2048], P('tp'), may hold values from 0.099609375 to 1.8984375
- mixout_weight: bfloat16 [2048, 4096], P('tp', 'kv'), may hold values from -0.125 to 0.125
- memory: float32 [128, 8, 128, 256], P('kv', 'tp'), may hold values from -0.6 to 0.6
- stabilizer: float32 [128, 8], P('kv', 'tp'), may hold values from -4 to 4
- second_gain: bfloat16 [4096], replicated, may hold values from 0.099609375 to 1.8984375
- second_gate: bfloat16 [4096, 11264], P(None, ('kv', 'tp')), may hold values from -0.09375 to 0.09375
- second_up: bfloat16 [4096, 11264], P(None, ('kv', 'tp')), may hold values from -0.09375 to 0.09375
- second_down: bfloat16 [11264, 4096], P(('kv', 'tp')), may hold values from -0.25 to 0.25
Outputs:
- layer_out: bfloat16 [128, 4096], P(None, ('kv', 'tp'))
- memory_next: float32 [128, 8, 128, 256], P('kv', 'tp')
- stabilizer_next: float32 [128, 8], P('kv', 'tp')
The draws below stay inside these ranges and needn't reach their ends.
All inputs are finite; a program needn't handle non-finite values.
Results may differ from the reference program's by a relative error of at most 0.013.
Values may be sent and summed in bfloat16 or wider, within the bound.
A program may use at most 64 MiB of HBM per device.

```python
import jax
import jax.numpy as jnp
from jax import lax

D = 4096
FF = 11264
H = 8
DK = 128
DV = 256
BATCH = 128


def draw_tokens(key, part):
    column = jnp.arange(D, dtype=jnp.float32)
    ramp = 0.5 * 4.0 ** (column / D)
    values = jax.random.normal(key, (BATCH, D), jnp.float32) * ramp[None, :]
    return jnp.clip(values, -12.0, 12.0).astype(jnp.bfloat16)


def with_spikes(result, key, source, target, parts, factor):
    owner, partner = [(jnp.arange(result.shape[position]) // (result.shape[position] // parts)).reshape([-1 if axis == position else 1 for axis in range(result.ndim)]) for position in (source, target)]
    chosen = jax.random.permutation(key, parts)[partner]
    strong = (owner == chosen) | (owner == (partner + parts // 2) % parts)
    return jnp.where(strong, factor * result, result)


def steps_of(key, shape, cuts, smallest, high):
    factor_of = 1.0
    for position, shards_of in cuts:
        steps = jax.random.uniform(jax.random.fold_in(jax.random.fold_in(key, 6), position), (shards_of,), jnp.float32, smallest / len(cuts), high / len(cuts))
        factor_of = factor_of * jnp.repeat(jnp.exp(steps), shape[position] // shards_of).reshape((-1,) + (1,) * (len(shape) - 1 - position))
    return factor_of


def gaussian(key, dims, spread, reach, cuts=(), kind=jnp.bfloat16):
    drawn = spread * jax.random.normal(key, dims, jnp.float32)
    if cuts:
        drawn = drawn * steps_of(key, dims, cuts, -0.22, 0.18)
    return jnp.clip(drawn, -reach, reach).astype(kind)


def bell_draw_with(key, extent, scale, most, shards, heavy, held_as=jnp.bfloat16):
    entries = scale * jax.random.normal(key, extent, jnp.float32)
    if shards:
        entries = entries * steps_of(key, extent, shards, -0.22, 0.18)
    return jnp.clip(with_spikes(entries, jax.random.fold_in(key, 3), *heavy), -most, most).astype(held_as)


def setup_inputs(seed: int = 0) -> dict:
    seeds = jax.random.split(jax.random.key(seed), 22)
    tokens = draw_tokens(jax.random.fold_in(seeds[21], 71), 0)
    first_gain = jnp.clip(1.0 + 0.18 * jax.random.normal(seeds[1], (D,), jnp.float32), 0.099609375, 1.8984375).astype(jnp.bfloat16)
    first_gate = gaussian(seeds[2], (D, FF), D ** -0.5, 0.09375, ((1, 256),))
    first_up = gaussian(seeds[3], (D, FF), D ** -0.5, 0.09375, ((1, 256),))
    first_down = bell_draw_with(seeds[4], (FF, D), FF ** -0.5, 0.25, ((0, 256),), (0, 1, 256, 6.0))
    mix_gain = jnp.clip(1.0 + 0.18 * jax.random.normal(seeds[5], (D,), jnp.float32), 0.099609375, 1.8984375).astype(jnp.bfloat16)
    query_weight = gaussian(seeds[6], (D, H * DK), D ** -0.5, 0.09375, ((0, 32), (1, 8)))
    key_weight = gaussian(seeds[7], (D, H * DK), D ** -0.5, 0.09375, ((0, 32), (1, 8)))
    value_weight = gaussian(seeds[8], (D, H * DV), D ** -0.5, 0.09375, ((0, 32), (1, 8)))
    outgate_weight = gaussian(seeds[9], (D, H * DV), D ** -0.5, 0.09375, ((0, 32), (1, 8)))
    ingate_weight = gaussian(seeds[10], (D, H), D ** -0.5, 0.09375, ((0, 32),))
    forget_weight = gaussian(seeds[11], (D, H), D ** -0.5, 0.09375, ((0, 32),))
    forget_bias = jnp.clip(-1.0 + 5.0 * jax.random.uniform(seeds[12], (H,), jnp.float32) ** steps_of(seeds[12], (H,), ((0, 8),), -0.2, 0.2), -1.0, 4.0)
    head_gain = jnp.clip(1.0 + 0.18 * jax.random.normal(seeds[13], (H * DV,), jnp.float32), 0.099609375, 1.8984375).astype(jnp.bfloat16)
    mixout_weight = gaussian(seeds[14], (H * DV, D), (H * DV) ** -0.5, 0.125, ((0, 8), (1, 32)))
    memory = gaussian(seeds[15], (BATCH, H, DK, DV), 0.1, 0.6, ((0, 32), (1, 8)), jnp.float32)
    stabilizer = gaussian(seeds[16], (BATCH, H), 1.0, 4.0, ((0, 32), (1, 8)), jnp.float32)
    second_gain = jnp.clip(1.0 + 0.18 * jax.random.normal(seeds[17], (D,), jnp.float32), 0.099609375, 1.8984375).astype(jnp.bfloat16)
    second_gate = gaussian(seeds[18], (D, FF), D ** -0.5, 0.09375, ((1, 256),))
    second_up = gaussian(seeds[19], (D, FF), D ** -0.5, 0.09375, ((1, 256),))
    second_down = bell_draw_with(seeds[20], (FF, D), FF ** -0.5, 0.25, ((0, 256),), (0, 1, 256, 6.0))
    return dict(tokens=tokens, first_gain=first_gain, first_gate=first_gate, first_up=first_up, first_down=first_down, mix_gain=mix_gain, query_weight=query_weight, key_weight=key_weight, value_weight=value_weight, outgate_weight=outgate_weight, ingate_weight=ingate_weight, forget_weight=forget_weight, forget_bias=forget_bias, head_gain=head_gain, mixout_weight=mixout_weight, memory=memory, stabilizer=stabilizer, second_gain=second_gain, second_gate=second_gate, second_up=second_up, second_down=second_down)


epsilon = 1e-06

def row_scale(wide_values):
    return lax.rsqrt(lax.optimization_barrier(jnp.mean(wide_values * wide_values, axis=-1, keepdims=True)) + epsilon)

def half_mlp(tokens, norm_gain, gate_weight, up_weight, down_weight):
    wide_tokens = tokens.astype(jnp.float32)
    row_factor = row_scale(wide_tokens)
    normed = (wide_tokens * norm_gain.astype(jnp.float32)).astype(jnp.bfloat16)
    gate_sum = row_factor * jnp.dot(normed, gate_weight, preferred_element_type=jnp.float32)
    up_sum = row_factor * jnp.dot(normed, up_weight, preferred_element_type=jnp.float32)
    hidden = (jax.nn.silu(gate_sum) * up_sum).astype(jnp.bfloat16)
    branch = jnp.dot(hidden, down_weight, preferred_element_type=jnp.float32)
    return (wide_tokens + 0.5 * branch).astype(jnp.bfloat16)

def reference(tokens, first_gain, first_gate, first_up, first_down, mix_gain, query_weight, key_weight, value_weight, outgate_weight, ingate_weight, forget_weight, forget_bias, head_gain, mixout_weight, memory, stabilizer, second_gain, second_gate, second_up, second_down):
    first = half_mlp(tokens, first_gain, first_gate, first_up, first_down)
    wide_first = first.astype(jnp.float32)
    row_factor = row_scale(wide_first)
    normed = (wide_first * mix_gain.astype(jnp.float32)).astype(jnp.bfloat16)
    rows_total = tokens.shape[0]

    def project(matrix):
        return row_factor * jnp.dot(normed, matrix, preferred_element_type=jnp.float32)
    query = project(query_weight).astype(jnp.bfloat16).reshape(rows_total, H, DK)
    keys = project(key_weight).astype(jnp.bfloat16).reshape(rows_total, H, DK)
    values = project(value_weight).astype(jnp.bfloat16).reshape(rows_total, H, DV)
    outgate = project(outgate_weight).astype(jnp.bfloat16).reshape(rows_total, H, DV)
    ingate = project(ingate_weight)
    forget = project(forget_weight) + forget_bias[None, :]
    log_forget = jax.nn.log_sigmoid(forget)
    ceiling = jnp.maximum(log_forget + stabilizer, ingate)
    retain = jnp.exp(log_forget + stabilizer - ceiling)
    admission = jnp.exp(ingate - ceiling)
    scaled_keys = keys.astype(jnp.float32) * DK ** (-0.5)
    outer_product = jnp.einsum('bhd,bhe->bhde', scaled_keys, values.astype(jnp.float32))
    memory_next = retain[..., None, None] * memory + admission[..., None, None] * outer_product
    readout = jnp.einsum('bhd,bhde->bhe', query.astype(jnp.float32), memory_next, precision=lax.Precision.HIGHEST)
    normalized = readout * lax.rsqrt(lax.optimization_barrier(jnp.mean(readout * readout, axis=-1, keepdims=True)) + epsilon)
    gated = normalized * head_gain.reshape(H, DV).astype(jnp.float32) * jax.nn.sigmoid(outgate.astype(jnp.float32))
    mixed = gated.reshape(rows_total, H * DV).astype(jnp.bfloat16)
    mix_branch = jnp.dot(mixed, mixout_weight, preferred_element_type=jnp.float32)
    after_mix = (wide_first + mix_branch).astype(jnp.bfloat16)
    layer_out = half_mlp(after_mix, second_gain, second_gate, second_up, second_down)
    return (layer_out, memory_next, ceiling)
```

```python
import functools

import jax
import jax.numpy as jnp
from jax import lax
from jax.experimental import pallas as pl
from jax.experimental.pallas import tpu as pltpu
from jax.sharding import PartitionSpec as P

EPS = 1e-06
Y = 4
C = 2
ROWS = 16
SEQ = 4
MESH = pl.DeviceIdType.MESH
bf16 = jnp.bfloat16
f32 = jnp.float32


def nothing():
    pass


def near_first(n):
    return sorted(range(n), key=lambda i: (min(i, n - i), i))


def hops(d, n):
    return min(d, n - d)


def remote(src, dst, send, recv, kv, tp):
    return pltpu.make_async_remote_copy(
        src_ref=src, dst_ref=dst, send_sem=send, recv_sem=recv, device_id=(kv, tp), device_id_type=MESH
    )


def wait_for(ref, sem):
    pltpu.make_async_copy(ref, ref, sem).wait()


def kernel(kv_size, tp_size, *refs):
    Z, X = kv_size // Y, tp_size // C
    YX, TP, B = Y * X, tp_size, SEQ * kv_size
    G = YX * C * ROWS
    D = Z * G
    FK = TP * ROWS
    near, far = near_first(Z), near_first(Z)[::-1]
    plane_far = sorted(range(1, YX), key=lambda p: -hops(p // X, Y) - hops(p % X, X))
    kv_far = sorted(range(1, kv_size), key=lambda p: -hops(p // Y, Z) - hops(p % Y, Y))

    args = (
        "tok", "g1", "wg1", "wu1", "wd1", "gm", "wq", "wk", "wv", "wo", "wi", "wf", "fb", "hg", "wm",
        "mem", "stab", "g2", "wg2", "wu2", "wd2",
    )
    names = args + ("out_o", "mem_o", "stab_o") + tuple(a + "_v" for a in args)
    names += ("gm32", "wmisc", "wmt", "tr", "hid")
    for k in "12":
        names += tuple(
            n + k
            for n in (
                "wgs", "wus", "wds", "wp", "dt", "xall", "ebuf", "erec", "sbuf", "prow", "zbuf", "zrec",
                "sw", "ssw", "az", "saz", "ap", "sap", "ex", "rp", "srp", "rz", "srz",
            )
        )
    names += ("fbuf", "sm", "yrec", "zb", "zr", "mm", "obuf", "of32", "orec", "lsem")
    names += ("fs", "my", "smy", "mz", "smz", "ns", "os")
    r = dict(zip(names, refs, strict=True))

    kv, tp = lax.axis_index("kv"), lax.axis_index("tp")
    z, y = kv // Y, kv % Y
    x, c = tp // C, tp % C
    yx = y * X + x
    other = 1 - c

    barrier = pltpu.get_barrier_semaphore()

    def greet(kv_to, tp_to):
        pl.semaphore_signal(barrier, inc=1, device_id=(kv_to, tp_to), device_id_type=MESH)

    for dz in range(1, Z):
        greet((z + dz) % Z * Y + y, tp)
    for p in range(1, YX):
        greet(z * Y + (y + p // X) % Y, (x + p % X) % X * C + c)
    for dx in range(X):
        greet(kv, (x + dx) % X * C + other)
    for p in kv_far:
        if p // Y and p % Y:
            greet((z + p // Y) % Z * Y + (y + p % Y) % Y, tp)

    copies = {
        n: pltpu.make_async_copy(r[n], r[n + "_v"], r["lsem"].at[i]) for i, n in enumerate(args)
    }
    for n in args:
        copies[n].start()

    for k in "12":
        r["xall" + k][:, :, other] = jnp.zeros((Z, YX, ROWS, B), bf16)
    r["hid"][...] = jnp.zeros_like(r["hid"])
    r["tr"][...] = jnp.zeros_like(r["tr"])
    r["wmisc"][...] = jnp.zeros_like(r["wmisc"])
    copies["tok"].wait()
    pl.semaphore_wait(barrier, (Z - 1) + (YX - 1) + X + (Z - 1) * (Y - 1))

    def plane(send):
        for p in plane_far:
            yt, xt = (y + p // X) % Y, (x + p % X) % X
            send(p, yt * X + xt, z * Y + yt, xt * C + c)

    def swap_weights(k):
        for i, n in enumerate(("wg", "wu", "wd")):
            copies[n + k].wait()
            remote(
                r[n + k + "_v"], r[n + "s" + k], r["ssw" + k].at[i], r["sw" + k].at[i], kv, x * C + other
            ).start()

    def prep_up(k):
        copies["g" + k].wait()
        for i, n in enumerate(("wgs", "wus")):
            wait_for(r[n + k], r["sw" + k].at[i])
        gain, wp = r[f"g{k}_v"][...].astype(f32).reshape(1, D), r["wp" + k]
        for j, n in enumerate((f"wg{k}_v", f"wu{k}_v", "wgs" + k, "wus" + k)):
            for zz in range(Z):
                cols = slice(zz * G, zz * G + G)
                wp[zz, 48 * j + 40 : 48 * j + 48, :] = jnp.zeros((8, G), bf16)
                wp[zz, 48 * j : 48 * j + 44, :] = (r[n][:, cols].astype(f32) * gain[:, cols]).astype(bf16)

    def prep_down(k):
        wait_for(r["wds" + k], r["sw" + k].at[2])
        tr, dt = r["tr"], r["dt" + k]
        for zz in range(Z):
            cols = slice(zz * G, zz * G + G)
            tr[0:44, :] = r[f"wd{k}_v"][:, cols].astype(f32)
            tr[48:92, :] = r["wds" + k][:, cols].astype(f32)
            dt[zz] = jnp.transpose(tr[...]).astype(bf16).reshape(YX, C, ROWS, 128)

    def mlp(k, after_sends, after_z, after_scatter):
        xall, ebuf, erec, sbuf, prow, zbuf, zrec = (
            r[n + k] for n in ("xall", "ebuf", "erec", "sbuf", "prow", "zbuf", "zrec")
        )
        az, ap, ex, rp, rz, saz, sap, srp, srz = (
            r[n + k] for n in ("az", "ap", "ex", "rp", "rz", "saz", "sap", "srp", "srz")
        )
        hid = r["hid"]

        def spread(i):
            def send(p, target, kv_to, tp_to):
                remote(xall.at[i, yx, c], xall.at[i, yx, c], sap.at[i], ap.at[i], kv_to, tp_to).start()

            plane(send)

        for dz in far:
            if dz:
                kv_to = (z + dz) % Z * Y + y
                remote(xall.at[0, yx, c], xall.at[dz, yx, c], saz.at[dz], az.at[dz], kv_to, tp).start()
        spread(0)
        after_sends()
        for i in near[1:]:
            wait_for(xall.at[i, yx, c], az.at[i])
            spread(i)
        after_z()

        squares = jnp.zeros((8, B), f32)
        sums = jnp.zeros((192, B), f32)
        for i in near:
            wait_for(prow.at[0, pl.ds(1, YX - 1)], ap.at[i])
            sums += jnp.dot(
                r["wp" + k][(z - i + Z) % Z], xall[i].reshape(G, B), preferred_element_type=f32
            )
            wide = xall[i, :, c].astype(f32)
            squares += jnp.sum((wide * wide).reshape(YX * ROWS // 8, 8, B), axis=0)
        ebuf[0:192] = sums
        ebuf[192:200] = squares
        both = remote(ebuf, erec, ex.at[0], ex.at[1], kv, x * C + other)
        both.start()
        both.wait_recv()
        squares = ebuf[192:200] + erec[192:200]
        factor = lax.rsqrt(jnp.sum(squares, axis=0, keepdims=True) / D + EPS)
        for mine, theirs in ((0, 96), (96, 0)):
            total = factor * (ebuf[mine : mine + 96] + erec[theirs : theirs + 96])
            gate, up = total[0:48], total[48:96]
            hid[mine // 2 : mine // 2 + 48] = (gate / (1.0 + jnp.exp(-gate)) * up).astype(bf16)

        for i in far:
            weight = r["dt" + k][(z + i) % Z, :, c].reshape(YX * ROWS, 128)
            terms = jnp.dot(weight, hid[...], preferred_element_type=f32)
            sbuf[i] = terms.reshape(YX, ROWS, B).astype(bf16)

            def send(p, target, kv_to, tp_to):
                remote(sbuf.at[i, target], prow.at[i, p], srp.at[i], rp.at[i], kv_to, tp_to).start()

            plane(send)
        after_scatter()

        total = None
        for i in far:
            wait_for(prow.at[i, pl.ds(1, YX - 1)], rp.at[i])
            total = jnp.sum(prow[i, 1:YX].astype(f32), axis=0) + sbuf[i, yx].astype(f32)
            if i:
                zbuf[i] = total
                kv_to = (z + i) % Z * Y + y
                remote(zbuf.at[i], zrec.at[i], srz.at[i], rz.at[i], kv_to, tp).start()
        for i in near[1:]:
            wait_for(zrec.at[i], rz.at[i])
            total = total + zrec[i]

        def drain():
            both.wait_send()
            for i, n in enumerate(("wgs", "wus", "wds")):
                wait_for(r[n + k], r["ssw" + k].at[i])
            for i in range(Z):
                if i:
                    wait_for(xall.at[0, yx, c], saz.at[i])
                    wait_for(zbuf.at[i], srz.at[i])
                wait_for(prow.at[i, pl.ds(1, YX - 1)], sap.at[i])
                wait_for(prow.at[i, pl.ds(1, YX - 1)], srp.at[i])

        return 0.5 * total, drain

    r["xall1"][0, yx, c] = r["tok_v"][...]

    def prep_mix():
        for n in ("gm", "wq", "wk", "wv", "wo", "wi", "wf", "fb", "hg", "wm", "mem", "stab"):
            copies[n].wait()
        heads = r["wi_v"].shape[0]
        r["wmisc"][0, 0:heads] = r["wi_v"][...]
        r["wmisc"][1, 0:heads] = r["wf_v"][...]
        r["gm32"][...] = r["gm_v"][...].astype(f32).reshape(1, D)
        r["wmt"][...] = jnp.transpose(r["wm_v"][...].astype(f32)).astype(bf16)

    def prep_first():
        prep_up("1")
        prep_down("1")

    def prep_second():
        swap_weights("2")
        prep_mix()
        prep_up("2")
        prep_down("2")

    half, drain1 = mlp("1", lambda: swap_weights("1"), prep_first, prep_second)
    first = (r["tok_v"][...].astype(f32) + half).astype(bf16)

    fbuf = r["fbuf"]
    fbuf[tp] = first
    for d in range(1, TP):
        remote(fbuf.at[tp], fbuf.at[tp], r["fs"].at[0], r["fs"].at[1], kv, (tp + d) % TP).start()
    wait_for(fbuf.at[pl.ds(1, TP - 1)], r["fs"].at[1])
    wide = jnp.transpose(fbuf[...].reshape(FK, B).astype(f32))
    row_squares = jnp.sum(wide * wide, axis=1, keepdims=True)
    gain = r["gm32"][:, pl.ds(pl.multiple_of(kv * FK, FK), FK)]
    w = (wide * gain).astype(bf16)

    def project(matrix):
        return jnp.dot(w, matrix, preferred_element_type=f32)

    def project_rows(matrix):
        return lax.dot_general(w, matrix, (((1,), (1,)), ((), ())), preferred_element_type=f32)

    lane = lax.broadcasted_iota(jnp.int32, (B, 128), 1)
    pieces = (
        project(r["wq_v"][...]),
        project(r["wk_v"][...]),
        project(r["wv_v"][:, 0:128]),
        project(r["wv_v"][:, 128:256]),
        project(r["wo_v"][:, 0:128]),
        project(r["wo_v"][:, 128:256]),
        jnp.where(lane == 8, row_squares, project_rows(r["wmisc"][0])),
        project_rows(r["wmisc"][1]),
    )
    sm = r["sm"]
    low = lax.broadcasted_iota(jnp.int32, (B // 8, 8, 128), 1) < 4
    for m in range(4):
        even, odd = (p.reshape(B // 8, 8, 128) for p in pieces[2 * m : 2 * m + 2])
        sm[:, 0, 8 * m : 8 * m + 8] = jnp.where(low, even, pltpu.roll(odd, 4, 1)).astype(bf16)
        sm[:, 1, 8 * m : 8 * m + 8] = jnp.where(low, pltpu.roll(even, 4, 1), odd).astype(bf16)

    yrec, zb, zr = r["yrec"], r["zb"], r["zr"]

    def seqs(kv_of):
        return kv_of // 2, kv_of % 2

    for i in far:
        zt = (z + i) % Z
        for dy in range(1, Y):
            a, b = seqs(zt * Y + (y + dy) % Y)
            remote(
                sm.at[a, b], yrec.at[i, dy], r["smy"].at[i], r["my"].at[i], z * Y + (y + dy) % Y, tp
            ).start()
    mine = None
    for i in far:
        wait_for(yrec.at[i, pl.ds(1, Y - 1)], r["my"].at[i])
        a, b = seqs((z + i) % Z * Y + y)
        mine = jnp.sum(yrec[i, 1:Y].astype(f32), axis=0) + sm[a, b].astype(f32)
        if i:
            zb[i] = mine.astype(bf16)
            remote(zb.at[i], zr.at[i], r["smz"].at[i], r["mz"].at[i], (z + i) % Z * Y + y, tp).start()
    for i in near[1:]:
        wait_for(zr.at[i], r["mz"].at[i])
        mine = mine + zr[i].astype(f32)

    lane8 = lax.broadcasted_iota(jnp.int32, (8, 128), 1)
    row8 = lax.broadcasted_iota(jnp.int32, (8, 128), 0)
    top = row8 < 4

    def rounded(v):
        return v.astype(bf16).astype(f32)

    def pick(v, at):
        return jnp.broadcast_to(jnp.sum(jnp.where(lane8 == at, v, 0.0), axis=1, keepdims=True), (8, 128))

    def both(v):
        return v + pltpu.roll(v, 4, 0)

    misc = mine[24:32]
    factor = lax.rsqrt(both(jnp.where(top, pick(misc, 8), 0.0)) / D + EPS)
    gates = pick(misc, tp) * factor
    ingate = jnp.where(top, gates, pltpu.roll(gates, 4, 0))
    forget = jnp.where(top, pltpu.roll(gates, 4, 0), gates) + r["fb_v"][...]
    spread4 = lax.broadcasted_iota(jnp.int32, (8, SEQ), 0) % SEQ == lax.broadcasted_iota(jnp.int32, (8, SEQ), 1)
    stab = jnp.sum(jnp.where(spread4, r["stab_v"][...], 0.0), axis=1, keepdims=True)
    log_forget = jnp.minimum(forget, 0.0) - jnp.log1p(jnp.exp(-jnp.abs(forget)))
    carried = log_forget + stab
    ceiling = jnp.maximum(carried, ingate)
    retain, admit = jnp.exp(carried - ceiling), jnp.exp(ingate - ceiling)
    diagonal = (row8 == lane8) & top
    r["stab_o"][...] = jnp.sum(jnp.where(diagonal, ceiling, 0.0), axis=0, keepdims=True)[:, 0:SEQ]

    qk = rounded(factor * mine[0:8])
    values = rounded(factor * mine[8:16])
    outgate = rounded(factor * mine[16:24])
    qk_cols = jnp.transpose(qk)
    scaled = 128**-0.5
    readout = jnp.zeros((8, 128), f32)
    for s in range(SEQ):
        q_col = jnp.broadcast_to(qk_cols[:, s : s + 1], (128, 128))
        k_col = jnp.broadcast_to(qk_cols[:, 4 + s : 5 + s] * scaled, (128, 128))
        for h in range(2):
            at = 4 * h + s
            old = r["mem_v"][s, 0, :, 128 * h : 128 * h + 128]
            new = retain[s : s + 1] * old + admit[s : s + 1] * (k_col * values[at : at + 1])
            r["mem_o"][s, 0, :, 128 * h : 128 * h + 128] = new
            readout = jnp.where(row8 == at, jnp.sum(q_col * new, axis=0, keepdims=True), readout)
    mean = both(jnp.broadcast_to(jnp.sum(readout * readout, axis=1, keepdims=True), (8, 128))) / 256
    hg = r["hg_v"]
    hg = hg[...].astype(f32).reshape(1, 256)
    head_gain = jnp.where(top, hg[:, 0:128], hg[:, 128:256])
    gated = readout * lax.rsqrt(mean + EPS) * head_gain / (1.0 + jnp.exp(-outgate))

    mm = r["mm"]
    mm[kv] = rounded(gated)
    for p in kv_far:
        kv_to = (z + p // Y) % Z * Y + (y + p % Y) % Y
        remote(mm.at[kv], mm.at[kv], r["ns"].at[0], r["ns"].at[1], kv_to, tp).start()
    others = mm.at[pl.ds(0, kv_size - 1)]
    wait_for(others, r["ns"].at[1])
    pairs = mm[...].reshape(B // 8, 2, 8, 128)
    a, b = pairs[:, 0], pairs[:, 1]
    left = jnp.where(low, a, pltpu.roll(b, 4, 1)).reshape(B, 128).astype(bf16)
    right = jnp.where(low, pltpu.roll(a, 4, 1), b).reshape(B, 128).astype(bf16)

    def across(m, v):
        return lax.dot_general(m, v, (((1,), (1,)), ((), ())), preferred_element_type=f32)

    terms = across(r["wmt"][:, 0:128], left) + across(r["wmt"][:, 128:256], right)
    terms = terms.reshape(TP, ROWS, B)
    r["of32"][...] = terms
    r["obuf"][...] = terms.astype(bf16)
    for d in range(1, TP):
        to = (tp + d) % TP
        remote(r["obuf"].at[to], r["orec"].at[d], r["os"].at[0], r["os"].at[1], kv, to).start()
    wait_for(r["orec"].at[pl.ds(1, TP - 1)], r["os"].at[1])
    branch = r["of32"][tp] + jnp.sum(r["orec"][1:TP].astype(f32), axis=0)
    after_mix = (first.astype(f32) + branch).astype(bf16)

    r["xall2"][0, yx, c] = after_mix
    half, drain2 = mlp("2", nothing, nothing, nothing)
    r["out_o"][...] = (after_mix.astype(f32) + half).astype(bf16)
    drain1()
    drain2()
    wait_for(fbuf.at[pl.ds(1, TP - 1)], r["fs"].at[0])
    wait_for(r["orec"].at[pl.ds(1, TP - 1)], r["os"].at[0])
    wait_for(others, r["ns"].at[0])
    for i in range(Z):
        wait_for(yrec.at[i, pl.ds(1, Y - 1)], r["smy"].at[i])
        if i:
            wait_for(zb.at[i], r["smz"].at[i])


def on_device(kv_size, tp_size, *args):
    (
        tokens, first_gain, first_gate, first_up, first_down, mix_gain,
        query_weight, key_weight, value_weight, outgate_weight, ingate_weight, forget_weight,
        forget_bias, head_gain, mixout_weight, memory, stabilizer,
        second_gain, second_gate, second_up, second_down,
    ) = args
    operands = (
        tokens.T, first_gain, first_gate.T, first_up.T, first_down, mix_gain,
        query_weight, key_weight, value_weight, outgate_weight, ingate_weight.T, forget_weight.T,
        forget_bias[None], head_gain, mixout_weight, memory, stabilizer.T,
        second_gain, second_gate.T, second_up.T, second_down,
    )
    Z, X = kv_size // Y, tp_size // C
    YX, TP, B = Y * X, tp_size, SEQ * kv_size
    G = YX * C * ROWS
    out_shapes = (
        jax.ShapeDtypeStruct((ROWS, B), bf16),
        jax.ShapeDtypeStruct(memory.shape, f32),
        jax.ShapeDtypeStruct((1, SEQ), f32),
    )
    DMA = pltpu.SemaphoreType.DMA
    raw = pltpu.VMEM(first_down.shape, bf16)
    block = (
        raw,
        raw,
        raw,
        pltpu.VMEM((Z, 192, G), bf16),
        pltpu.VMEM((Z, YX, C, ROWS, 128), bf16),
        pltpu.VMEM((Z, YX, C, ROWS, B), bf16),
        pltpu.VMEM((200, B), f32),
        pltpu.VMEM((200, B), f32),
        pltpu.VMEM((Z, YX, ROWS, B), bf16),
        pltpu.VMEM((Z, YX, ROWS, B), bf16),
        pltpu.VMEM((Z, ROWS, B), f32),
        pltpu.VMEM((Z, ROWS, B), f32),
        DMA((3,)),
        DMA((3,)),
        DMA((Z,)),
        DMA((Z,)),
        DMA((Z,)),
        DMA((Z,)),
        DMA((2,)),
        DMA((Z,)),
        DMA((Z,)),
        DMA((Z,)),
        DMA((Z,)),
    )
    scratch = (
        *(pltpu.VMEM(o.shape, o.dtype) for o in operands),
        pltpu.VMEM((1, mix_gain.shape[0]), f32),
        pltpu.VMEM((2, 128, TP * ROWS), bf16),
        pltpu.VMEM((TP * ROWS, 256), bf16),
        pltpu.VMEM((128, G), f32),
        pltpu.VMEM((128, B), bf16),
        *block,
        *block,
        pltpu.VMEM((TP, ROWS, B), bf16),
        pltpu.VMEM((kv_size // 2, 2, 32, 128), bf16),
        pltpu.VMEM((Z, Y, 32, 128), bf16),
        pltpu.VMEM((Z, 32, 128), bf16),
        pltpu.VMEM((Z, 32, 128), bf16),
        pltpu.VMEM((kv_size, 8, 128), f32),
        pltpu.VMEM((TP, ROWS, B), bf16),
        pltpu.VMEM((TP, ROWS, B), f32),
        pltpu.VMEM((TP, ROWS, B), bf16),
        DMA((len(operands),)),
        DMA((2,)),
        DMA((Z,)),
        DMA((Z,)),
        DMA((Z,)),
        DMA((Z,)),
        DMA((2,)),
        DMA((2,)),
    )
    out, memory_next, stabilizer_next = pl.pallas_call(
        functools.partial(kernel, kv_size, tp_size),
        out_shape=out_shapes,
        in_specs=[pl.BlockSpec(memory_space=pl.ANY)] * len(operands),
        out_specs=[pl.BlockSpec(memory_space=pltpu.VMEM)] * 3,
        scratch_shapes=scratch,
        compiler_params=pltpu.CompilerParams(
            collective_id=0, has_side_effects=True, vmem_limit_bytes=60 * 1024 * 1024
        ),
        name="decode_step",
    )(*operands)
    return out.T, memory_next, stabilizer_next.T


def solution(mesh):
    in_specs = (
        P(None, ("kv", "tp")),
        P(),
        P(None, ("kv", "tp")),
        P(None, ("kv", "tp")),
        P(("kv", "tp"), None),
        P(),
        P("kv", "tp"),
        P("kv", "tp"),
        P("kv", "tp"),
        P("kv", "tp"),
        P("kv", None),
        P("kv", None),
        P("tp"),
        P("tp"),
        P("tp", "kv"),
        P("kv", "tp", None, None),
        P("kv", "tp"),
        P(),
        P(None, ("kv", "tp")),
        P(None, ("kv", "tp")),
        P(("kv", "tp"), None),
    )
    out_specs = (P(None, ("kv", "tp")), P("kv", "tp", None, None), P("kv", "tp"))
    return jax.shard_map(
        functools.partial(on_device, mesh.shape["kv"], mesh.shape["tp"]),
        mesh=mesh,
        in_specs=in_specs,
        out_specs=out_specs,
        check_vma=False,
    )
```

```python
import functools

import jax
import jax.numpy as jnp
from jax import lax
from jax.experimental import pallas as pl
from jax.experimental.pallas import tpu as pltpu
from jax.sharding import PartitionSpec as P

EPS = 1e-06
Y = 4
C = 2
ROWS = 16
SEQ = 4
AG_GROUPS = ((0,), (3, 4), (5, 6, 7))
AG_DIRECT = (1, 2)
AG_ORDER = ((0,), (1,), (2,), (3, 4), (5, 6, 7))
RS_ORDER = ((1,), (2,), (7,), (5,), (6,), (3,), (4,), (0,))
RS_DIRECT = ()
RS_FIRST = (1, 2)
AG_LATE = ()
KS_DIRECT = (5, 6, 7)
MESH = pl.DeviceIdType.MESH
bf16 = jnp.bfloat16
f32 = jnp.float32


def nothing():
    pass


def near_first(n):
    return sorted(range(n), key=lambda i: (min(i, n - i), i))


def hops(d, n):
    return min(d, n - d)


def remote(src, dst, send, recv, kv, tp):
    return pltpu.make_async_remote_copy(
        src_ref=src, dst_ref=dst, send_sem=send, recv_sem=recv, device_id=(kv, tp), device_id_type=MESH
    )


def wait_for(ref, sem):
    pltpu.make_async_copy(ref, ref, sem).wait()


def kernel(kv_size, tp_size, *refs):
    Z, X = kv_size // Y, tp_size // C
    YX, TP, B = Y * X, tp_size, SEQ * kv_size
    G = YX * C * ROWS
    D = Z * G
    FK = TP * ROWS
    near, far = near_first(Z), near_first(Z)[::-1]
    plane_far = sorted(range(1, YX), key=lambda p: -hops(p // X, Y) - hops(p % X, X))
    kv_far = sorted(range(1, kv_size), key=lambda p: -hops(p // Y, Z) - hops(p % Y, Y))

    args = (
        "tok", "g1", "wg1", "wu1", "wd1", "gm", "wq", "wk", "wv", "wo", "wi", "wf", "fb", "hg", "wm",
        "mem", "stab", "g2", "wg2", "wu2", "wd2",
    )
    names = args + ("out_o", "mem_o", "stab_o") + tuple(a + "_v" for a in args)
    names += ("gm32", "wmisc", "wmt", "tr", "hid")
    for k in "12":
        names += tuple(
            n + k
            for n in (
                "wgs", "wus", "wds", "wp", "dt", "xall", "ebuf", "erec", "sbuf", "prow", "drow", "first", "zbuf", "zrec",
                "sw", "ssw", "az", "saz", "ap", "sap", "ex", "rp", "srp", "rz", "srz",
            )
        )
    names += ("fbuf", "sm", "yrec", "zb", "zr", "mm", "obuf", "of32", "orec", "lsem")
    names += ("fs", "my", "smy", "mz", "smz", "ns", "os")
    r = dict(zip(names, refs, strict=True))

    kv, tp = lax.axis_index("kv"), lax.axis_index("tp")
    z, y = kv // Y, kv % Y
    x, c = tp // C, tp % C
    yx = y * X + x
    other = 1 - c

    copies = {
        n: pltpu.make_async_copy(r[n], r[n + "_v"], r["lsem"].at[i]) for i, n in enumerate(args)
    }
    copies["tok"].start()

    peers = {(dz, 0, 0, 0) for dz in range(Z)} | {(dz, dy, 0, 0) for dz in range(Z) for dy in range(Y)}
    peers |= {(near[n], dy, dx, 0) for n in {0} | set(AG_DIRECT) | set(RS_DIRECT) for dy in range(Y) for dx in range(X)}
    peers |= {(0, 0, dx, dc) for dx in range(X) for dc in range(C)}
    peers -= {(0, 0, 0, 0)}
    barrier = pltpu.get_barrier_semaphore()
    for dz, dy, dx, dc in sorted(peers, key=lambda o: (-hops(o[0], Z) - hops(o[1], Y) - hops(o[2], X), o)):
        to = ((z + dz) % Z * Y + (y + dy) % Y, (x + dx) % X * C + (c + dc) % C)
        pl.semaphore_signal(barrier, inc=1, device_id=to, device_id_type=MESH)

    for n in args:
        if n != "tok":
            copies[n].start()

    copies["tok"].wait()
    r["xall1"][yx, c, 0] = r["tok_v"][...]
    pl.semaphore_wait(barrier, len(peers))

    def clear():
        for k in "12":
            r["xall" + k][:, other] = jnp.zeros((YX, Z, ROWS, B), bf16)
        r["hid"][...] = jnp.zeros_like(r["hid"])
        r["tr"][...] = jnp.zeros_like(r["tr"])
        r["wmisc"][...] = jnp.zeros_like(r["wmisc"])

    def plane(send, dz=0):
        for p in plane_far if dz == 0 else [*plane_far, 0]:
            yt, xt = (y + p // X) % Y, (x + p % X) % X
            send(p, yt * X + xt, (z + dz) % Z * Y + yt, xt * C + c)

    def swap_weights(k):
        for i, n in enumerate(("wg", "wu", "wd")):
            copies[n + k].wait()
            remote(
                r[n + k + "_v"], r[n + "s" + k], r["ssw" + k].at[i], r["sw" + k].at[i], kv, x * C + other
            ).start()

    def prep_up(k):
        copies["g" + k].wait()
        for i, n in enumerate(("wgs", "wus")):
            wait_for(r[n + k], r["sw" + k].at[i])
        gain, wp = r[f"g{k}_v"][...].astype(f32).reshape(1, D), r["wp" + k]
        for j, n in enumerate((f"wg{k}_v", f"wu{k}_v", "wgs" + k, "wus" + k)):
            for zz in range(Z):
                cols = slice(zz * G, zz * G + G)
                wp[zz, 48 * j + 40 : 48 * j + 48, :] = jnp.zeros((8, G), bf16)
                wp[zz, 48 * j : 48 * j + 44, :] = (r[n][:, cols].astype(f32) * gain[:, cols]).astype(bf16)

    def prep_down(k):
        wait_for(r["wds" + k], r["sw" + k].at[2])
        tr, dt = r["tr"], r["dt" + k]
        for zz in range(Z):
            cols = slice(zz * G, zz * G + G)
            tr[0:44, :] = r[f"wd{k}_v"][:, cols].astype(f32)
            tr[48:92, :] = r["wds" + k][:, cols].astype(f32)
            dt[zz] = jnp.transpose(tr[...]).astype(bf16).reshape(YX, C, ROWS, 128)

    def mlp(k, after_sends, after_z, before_last):
        xall, ebuf, erec, sbuf, prow, drow, first, zbuf, zrec = (
            r[n + k] for n in ("xall", "ebuf", "erec", "sbuf", "prow", "drow", "first", "zbuf", "zrec")
        )
        az, ap, ex, rp, rz, saz, sap, srp, srz = (
            r[n + k] for n in ("az", "ap", "ex", "rp", "rz", "saz", "sap", "srp", "srz")
        )
        hid = r["hid"]

        def at_z(n):
            return (z + near[n]) % Z * Y + y

        def blocks(n, first):
            return prow.at[pl.ds(first, YX - first), pl.ds(0, n)]

        def spread(group):
            part = xall.at[yx, c, pl.ds(group[0], len(group))]

            def send(p, target, kv_to, tp_to):
                remote(part, part, sap.at[group[0]], ap.at[group[0]], kv_to, tp_to).start()

            plane(send)

        def spread_direct(n):
            mine, there = xall.at[yx, c, 0], xall.at[yx, c, n]

            def send(p, target, kv_to, tp_to):
                remote(mine, there, sap.at[n], ap.at[n], kv_to, tp_to).start()

            plane(send, near[n])

        for n in range(Z)[::-1]:
            if n and n not in AG_DIRECT and n not in AG_LATE:
                remote(xall.at[yx, c, 0], xall.at[yx, c, n], saz.at[n], az.at[n], at_z(n), tp).start()
        spread(AG_GROUPS[0])
        for n in AG_DIRECT:
            spread_direct(n)
        after_sends()
        for group in AG_GROUPS[1:]:
            for n in group:
                wait_for(xall.at[yx, c, n], az.at[n])
            spread(group)
        after_z()

        squares = jnp.zeros((8, B), f32)
        sums = jnp.zeros((192, B), f32)
        for group in AG_ORDER:
            if group[0] in AG_LATE:
                wait_for(xall.at[:, c, group[0]], az.at[group[0]])
            else:
                wait_for(blocks(len(group), 0 if group[0] in AG_DIRECT else 1), ap.at[group[0]])
            if group[0] == 0:
                for n in AG_LATE:
                    remote(xall.at[:, c, 0], xall.at[:, c, n], saz.at[n], az.at[n], at_z(n), tp).start()
            for n in group:
                rows = xall[:, :, n].reshape(G, B)
                sums += jnp.dot(r["wp" + k][(z - near[n] + Z) % Z], rows, preferred_element_type=f32)
                wide = xall[:, c, n].astype(f32)
                squares += jnp.sum((wide * wide).reshape(YX * ROWS // 8, 8, B), axis=0)
        ebuf[0:192] = sums
        ebuf[192:200] = squares
        both = remote(ebuf, erec, ex.at[0], ex.at[1], kv, x * C + other)
        both.start()
        both.wait_recv()
        squares = ebuf[192:200] + erec[192:200]
        factor = lax.rsqrt(jnp.sum(squares, axis=0, keepdims=True) / D + EPS)
        for mine, theirs in ((0, 96), (96, 0)):
            total = factor * (ebuf[mine : mine + 96] + erec[theirs : theirs + 96])
            gate, up = total[0:48], total[48:96]
            hid[mine // 2 : mine // 2 + 48] = (gate / (1.0 + jnp.exp(-gate)) * up).astype(bf16)

        for group in RS_ORDER:
            for n in group:
                weight = r["dt" + k][(z + near[n]) % Z, :, c].reshape(YX * ROWS, 128)
                terms = jnp.dot(weight, hid[...], preferred_element_type=f32).reshape(YX, ROWS, B)
                if n == 0:
                    before_last()
                    for at, m in enumerate(RS_FIRST):
                        wait_for(first.at[at], rz.at[m])
                        terms += first[at].astype(f32)
                sbuf[:, n] = terms.astype(bf16)
            n = group[0]
            if n in RS_FIRST:
                at = RS_FIRST.index(n)
                remote(sbuf.at[:, n], first.at[at], srz.at[n], rz.at[n], at_z(n), tp).start()
                continue
            if n in RS_DIRECT:
                at = RS_DIRECT.index(n)

                def send(p, target, kv_to, tp_to):
                    remote(sbuf.at[target, n], drow.at[at, p], srp.at[n], rp.at[n], kv_to, tp_to).start()

                plane(send, near[n])
            else:
                some = pl.ds(n, len(group))

                def send(p, target, kv_to, tp_to):
                    remote(
                        sbuf.at[target, some], prow.at[p, some], srp.at[n], rp.at[n], kv_to, tp_to
                    ).start()

                plane(send)

        total = jnp.zeros((ROWS, B), f32)
        for group in RS_ORDER:
            if group[0] in RS_DIRECT or group[0] in RS_FIRST:
                continue
            wait_for(blocks(len(group), 1), rp.at[group[0]])
            for n in group[::-1]:
                part = jnp.sum(prow[1:YX, n].astype(f32), axis=0) + sbuf[yx, n].astype(f32)
                if n:
                    zbuf[n] = part
                    remote(zbuf.at[n], zrec.at[n], srz.at[n], rz.at[n], at_z(n), tp).start()
                else:
                    total += part
        for n in RS_DIRECT:
            wait_for(drow.at[RS_DIRECT.index(n)], rp.at[n])
            total += jnp.sum(drow[RS_DIRECT.index(n)].astype(f32), axis=0)
        for n in range(1, Z):
            if n not in RS_DIRECT and n not in RS_FIRST:
                wait_for(zrec.at[n], rz.at[n])
                total += zrec[n]

        def drain():
            both.wait_send()
            for i, n in enumerate(("wgs", "wus", "wds")):
                wait_for(r[n + k], r["ssw" + k].at[i])
            for n in range(1, Z):
                if n in AG_LATE:
                    wait_for(xall.at[:, c, n], saz.at[n])
                elif n not in AG_DIRECT:
                    wait_for(xall.at[yx, c, n], saz.at[n])
                if n in RS_FIRST:
                    wait_for(sbuf.at[:, n], srz.at[n])
                elif n not in RS_DIRECT:
                    wait_for(zbuf.at[n], srz.at[n])
            for order, direct, sem in ((AG_ORDER, AG_DIRECT, sap), (RS_ORDER, RS_DIRECT, srp)):
                for group in order:
                    if group[0] in (AG_LATE if sem is sap else RS_FIRST):
                        continue
                    wait_for(blocks(len(group), 0 if group[0] in direct else 1), sem.at[group[0]])

        return 0.5 * total, drain


    def prep_mix():
        for n in ("gm", "wq", "wk", "wv", "wo", "wi", "wf", "fb", "hg", "wm", "mem", "stab"):
            copies[n].wait()
        heads = r["wi_v"].shape[0]
        r["wmisc"][0, 0:heads] = r["wi_v"][...]
        r["wmisc"][1, 0:heads] = r["wf_v"][...]
        r["gm32"][...] = r["gm_v"][...].astype(f32).reshape(1, D)
        r["wmt"][...] = jnp.transpose(r["wm_v"][...].astype(f32)).astype(bf16)

    def prep_first():
        prep_up("1")
        prep_down("1")

    def start_first():
        swap_weights("1")
        clear()

    def before_mix():
        swap_weights("2")
        prep_mix()

    def prep_second():
        prep_up("2")
        prep_down("2")

    half, drain1 = mlp("1", start_first, prep_first, before_mix)
    first = (r["tok_v"][...].astype(f32) + half).astype(bf16)

    fbuf = r["fbuf"]
    fbuf[tp] = first
    for d in range(1, TP):
        remote(fbuf.at[tp], fbuf.at[tp], r["fs"].at[0], r["fs"].at[1], kv, (tp + d) % TP).start()
    wait_for(fbuf.at[pl.ds(1, TP - 1)], r["fs"].at[1])
    wide = jnp.transpose(fbuf[...].reshape(FK, B).astype(f32))
    row_squares = jnp.sum(wide * wide, axis=1, keepdims=True)
    gain = r["gm32"][:, pl.ds(pl.multiple_of(kv * FK, FK), FK)]
    w = (wide * gain).astype(bf16)

    def project(matrix):
        return jnp.dot(w, matrix, preferred_element_type=f32)

    def project_rows(matrix):
        return lax.dot_general(w, matrix, (((1,), (1,)), ((), ())), preferred_element_type=f32)

    lane = lax.broadcasted_iota(jnp.int32, (B, 128), 1)
    pieces = (
        project(r["wq_v"][...]),
        project(r["wk_v"][...]),
        project(r["wv_v"][:, 0:128]),
        project(r["wv_v"][:, 128:256]),
        project(r["wo_v"][:, 0:128]),
        project(r["wo_v"][:, 128:256]),
        jnp.where(lane == 8, row_squares, project_rows(r["wmisc"][0])),
        project_rows(r["wmisc"][1]),
    )
    sm = r["sm"]
    low = lax.broadcasted_iota(jnp.int32, (B // 8, 8, 128), 1) < 4
    for m in range(4):
        even, odd = (p.reshape(B // 8, 8, 128) for p in pieces[2 * m : 2 * m + 2])
        sm[:, 0, 8 * m : 8 * m + 8] = jnp.where(low, even, pltpu.roll(odd, 4, 1)).astype(bf16)
        sm[:, 1, 8 * m : 8 * m + 8] = jnp.where(low, pltpu.roll(even, 4, 1), odd).astype(bf16)

    yrec, zb, zr = r["yrec"], r["zb"], r["zr"]

    def seqs(kv_of):
        return kv_of // 2, kv_of % 2

    def to_kv(n, dy):
        return (z + near[n]) % Z * Y + (y + dy) % Y

    for n in range(Z)[::-1]:
        for dy in range(Y)[::-1]:
            if dy or n in KS_DIRECT:
                to = to_kv(n, dy)
                through = to if n in KS_DIRECT else to_kv(0, dy)
                a, b = seqs(to)
                remote(sm.at[a, b], yrec.at[n, dy], r["smy"].at[n], r["my"].at[n], through, tp).start()
    mine = jnp.zeros((32, 128), f32)
    for n in range(Z)[::-1]:
        if n in KS_DIRECT:
            continue
        wait_for(yrec.at[n, pl.ds(1, Y - 1)], r["my"].at[n])
        a, b = seqs(to_kv(n, 0))
        part = jnp.sum(yrec[n, 1:Y].astype(f32), axis=0) + sm[a, b].astype(f32)
        if n:
            zb[n] = part.astype(bf16)
            remote(zb.at[n], zr.at[n], r["smz"].at[n], r["mz"].at[n], to_kv(n, 0), tp).start()
        else:
            mine += part
    for n in range(1, Z):
        if n in KS_DIRECT:
            wait_for(yrec.at[n], r["my"].at[n])
            mine += jnp.sum(yrec[n].astype(f32), axis=0)
        else:
            wait_for(zr.at[n], r["mz"].at[n])
            mine += zr[n].astype(f32)

    lane8 = lax.broadcasted_iota(jnp.int32, (8, 128), 1)
    row8 = lax.broadcasted_iota(jnp.int32, (8, 128), 0)
    top = row8 < 4

    def rounded(v):
        return v.astype(bf16).astype(f32)

    def pick(v, at):
        return jnp.broadcast_to(jnp.sum(jnp.where(lane8 == at, v, 0.0), axis=1, keepdims=True), (8, 128))

    def both(v):
        return v + pltpu.roll(v, 4, 0)

    misc = mine[24:32]
    factor = lax.rsqrt(both(jnp.where(top, pick(misc, 8), 0.0)) / D + EPS)
    gates = pick(misc, tp) * factor
    ingate = jnp.where(top, gates, pltpu.roll(gates, 4, 0))
    forget = jnp.where(top, pltpu.roll(gates, 4, 0), gates) + r["fb_v"][...]
    spread4 = lax.broadcasted_iota(jnp.int32, (8, SEQ), 0) % SEQ == lax.broadcasted_iota(jnp.int32, (8, SEQ), 1)
    stab = jnp.sum(jnp.where(spread4, r["stab_v"][...], 0.0), axis=1, keepdims=True)
    log_forget = jnp.minimum(forget, 0.0) - jnp.log1p(jnp.exp(-jnp.abs(forget)))
    carried = log_forget + stab
    ceiling = jnp.maximum(carried, ingate)
    retain, admit = jnp.exp(carried - ceiling), jnp.exp(ingate - ceiling)
    diagonal = (row8 == lane8) & top
    r["stab_o"][...] = jnp.sum(jnp.where(diagonal, ceiling, 0.0), axis=0, keepdims=True)[:, 0:SEQ]

    qk = rounded(factor * mine[0:8])
    values = rounded(factor * mine[8:16])
    outgate = rounded(factor * mine[16:24])
    qk_cols = jnp.transpose(qk)
    scaled = 128**-0.5
    readout = jnp.zeros((8, 128), f32)
    for s in range(SEQ):
        q_col = jnp.broadcast_to(qk_cols[:, s : s + 1], (128, 128))
        k_col = jnp.broadcast_to(qk_cols[:, 4 + s : 5 + s] * scaled, (128, 128))
        for h in range(2):
            at = 4 * h + s
            old = r["mem_v"][s, 0, :, 128 * h : 128 * h + 128]
            new = retain[s : s + 1] * old + admit[s : s + 1] * (k_col * values[at : at + 1])
            r["mem_o"][s, 0, :, 128 * h : 128 * h + 128] = new
            readout = jnp.where(row8 == at, jnp.sum(q_col * new, axis=0, keepdims=True), readout)
    mean = both(jnp.broadcast_to(jnp.sum(readout * readout, axis=1, keepdims=True), (8, 128))) / 256
    hg = r["hg_v"]
    hg = hg[...].astype(f32).reshape(1, 256)
    head_gain = jnp.where(top, hg[:, 0:128], hg[:, 128:256])
    gated = readout * lax.rsqrt(mean + EPS) * head_gain / (1.0 + jnp.exp(-outgate))

    mm = r["mm"]
    mm[kv] = gated.astype(bf16)
    for p in kv_far:
        kv_to = (z + p // Y) % Z * Y + (y + p % Y) % Y
        remote(mm.at[kv], mm.at[kv], r["ns"].at[0], r["ns"].at[1], kv_to, tp).start()
    prep_second()
    others = mm.at[pl.ds(0, kv_size - 1)]
    wait_for(others, r["ns"].at[1])
    pairs = mm[...].astype(f32).reshape(B // 8, 2, 8, 128)
    a, b = pairs[:, 0], pairs[:, 1]
    left = jnp.where(low, a, pltpu.roll(b, 4, 1)).reshape(B, 128).astype(bf16)
    right = jnp.where(low, pltpu.roll(a, 4, 1), b).reshape(B, 128).astype(bf16)

    def across(m, v):
        return lax.dot_general(m, v, (((1,), (1,)), ((), ())), preferred_element_type=f32)

    terms = across(r["wmt"][:, 0:128], left) + across(r["wmt"][:, 128:256], right)
    terms = terms.reshape(TP, ROWS, B)
    r["of32"][...] = terms
    r["obuf"][...] = terms.astype(bf16)
    for d in range(1, TP):
        to = (tp + d) % TP
        remote(r["obuf"].at[to], r["orec"].at[d], r["os"].at[0], r["os"].at[1], kv, to).start()
    wait_for(r["orec"].at[pl.ds(1, TP - 1)], r["os"].at[1])
    branch = r["of32"][tp] + jnp.sum(r["orec"][1:TP].astype(f32), axis=0)
    after_mix = (first.astype(f32) + branch).astype(bf16)

    r["xall2"][yx, c, 0] = after_mix
    half, drain2 = mlp("2", nothing, nothing, nothing)
    r["out_o"][...] = (after_mix.astype(f32) + half).astype(bf16)
    drain1()
    drain2()
    wait_for(fbuf.at[pl.ds(1, TP - 1)], r["fs"].at[0])
    wait_for(r["orec"].at[pl.ds(1, TP - 1)], r["os"].at[0])
    wait_for(others, r["ns"].at[0])
    for n in range(Z):
        if n in KS_DIRECT:
            wait_for(yrec.at[n], r["smy"].at[n])
        else:
            wait_for(yrec.at[n, pl.ds(1, Y - 1)], r["smy"].at[n])
            if n:
                wait_for(zb.at[n], r["smz"].at[n])


def finish(*refs):
    source, target, held, sems = refs[0:3], refs[3:6], refs[6:9], refs[9]
    parts = [(1, i) for i in range(SEQ)] + [(0, None), (2, None)]

    def at(refs, k):
        which, i = parts[k]
        return refs[which] if i is None else refs[which].at[i]

    ins = [pltpu.make_async_copy(at(source, k), at(held, k), sems.at[0, k]) for k in range(6)]
    outs = [pltpu.make_async_copy(at(held, k), at(target, k), sems.at[1, k]) for k in range(6)]
    for copy in ins:
        copy.start()
    for copy, out in zip(ins, outs):
        copy.wait()
        out.start()
    for out in outs:
        out.wait()


def on_device(kv_size, tp_size, *args):
    (
        tokens, first_gain, first_gate, first_up, first_down, mix_gain,
        query_weight, key_weight, value_weight, outgate_weight, ingate_weight, forget_weight,
        forget_bias, head_gain, mixout_weight, memory, stabilizer,
        second_gain, second_gate, second_up, second_down,
    ) = args
    operands = (
        tokens.T, first_gain, first_gate.T, first_up.T, first_down, mix_gain,
        query_weight, key_weight, value_weight, outgate_weight, ingate_weight.T, forget_weight.T,
        forget_bias[None], head_gain, mixout_weight, memory, stabilizer.T,
        second_gain, second_gate.T, second_up.T, second_down,
    )
    Z, X = kv_size // Y, tp_size // C
    YX, TP, B = Y * X, tp_size, SEQ * kv_size
    G = YX * C * ROWS
    out_shapes = (
        jax.ShapeDtypeStruct((ROWS, B), bf16),
        jax.ShapeDtypeStruct(memory.shape, f32),
        jax.ShapeDtypeStruct((1, SEQ), f32),
    )
    DMA = pltpu.SemaphoreType.DMA
    raw = pltpu.VMEM(first_down.shape, bf16)
    block = (
        raw,
        raw,
        raw,
        pltpu.VMEM((Z, 192, G), bf16),
        pltpu.VMEM((Z, YX, C, ROWS, 128), bf16),
        pltpu.VMEM((YX, C, Z, ROWS, B), bf16),
        pltpu.VMEM((200, B), f32),
        pltpu.VMEM((200, B), f32),
        pltpu.VMEM((YX, Z, ROWS, B), bf16),
        pltpu.VMEM((YX, Z, ROWS, B), bf16),
        pltpu.VMEM((max(1, len(RS_DIRECT)), YX, ROWS, B), bf16),
        pltpu.VMEM((max(1, len(RS_FIRST)), YX, ROWS, B), bf16),
        pltpu.VMEM((Z, ROWS, B), f32),
        pltpu.VMEM((Z, ROWS, B), f32),
        DMA((3,)),
        DMA((3,)),
        DMA((Z,)),
        DMA((Z,)),
        DMA((Z,)),
        DMA((Z,)),
        DMA((2,)),
        DMA((Z,)),
        DMA((Z,)),
        DMA((Z,)),
        DMA((Z,)),
    )
    scratch = (
        *(pltpu.VMEM(o.shape, o.dtype) for o in operands),
        pltpu.VMEM((1, mix_gain.shape[0]), f32),
        pltpu.VMEM((2, 128, TP * ROWS), bf16),
        pltpu.VMEM((TP * ROWS, 256), bf16),
        pltpu.VMEM((128, G), f32),
        pltpu.VMEM((128, B), bf16),
        *block,
        *block,
        pltpu.VMEM((TP, ROWS, B), bf16),
        pltpu.VMEM((kv_size // 2, 2, 32, 128), bf16),
        pltpu.VMEM((Z, Y, 32, 128), bf16),
        pltpu.VMEM((Z, 32, 128), bf16),
        pltpu.VMEM((Z, 32, 128), bf16),
        pltpu.VMEM((kv_size, 8, 128), bf16),
        pltpu.VMEM((TP, ROWS, B), bf16),
        pltpu.VMEM((TP, ROWS, B), f32),
        pltpu.VMEM((TP, ROWS, B), bf16),
        DMA((len(operands),)),
        DMA((2,)),
        DMA((Z,)),
        DMA((Z,)),
        DMA((Z,)),
        DMA((Z,)),
        DMA((2,)),
        DMA((2,)),
    )
    out, memory_next, stabilizer_next = pl.pallas_call(
        functools.partial(kernel, kv_size, tp_size),
        out_shape=out_shapes,
        in_specs=[pl.BlockSpec(memory_space=pl.ANY)] * len(operands),
        out_specs=[pl.BlockSpec(memory_space=pltpu.VMEM)] * 3,
        scratch_shapes=scratch,
        compiler_params=pltpu.CompilerParams(
            collective_id=0, has_side_effects=True, vmem_limit_bytes=60 * 1024 * 1024
        ),
        name="decode_step",
    )(*operands)
    out, memory_next, stabilizer_next = pl.pallas_call(
        finish,
        out_shape=out_shapes,
        in_specs=[pl.BlockSpec(memory_space=pl.ANY)] * 3,
        out_specs=[pl.BlockSpec(memory_space=pl.ANY)] * 3,
        scratch_shapes=[*(pltpu.VMEM(o.shape, o.dtype) for o in out_shapes), DMA((2, 6))],
        compiler_params=pltpu.CompilerParams(vmem_limit_bytes=60 * 1024 * 1024),
        name="finish",
    )(out, memory_next, stabilizer_next)
    return out.T, memory_next, stabilizer_next.T


def solution(mesh):
    in_specs = (
        P(None, ("kv", "tp")),
        P(),
        P(None, ("kv", "tp")),
        P(None, ("kv", "tp")),
        P(("kv", "tp"), None),
        P(),
        P("kv", "tp"),
        P("kv", "tp"),
        P("kv", "tp"),
        P("kv", "tp"),
        P("kv", None),
        P("kv", None),
        P("tp"),
        P("tp"),
        P("tp", "kv"),
        P("kv", "tp", None, None),
        P("kv", "tp"),
        P(),
        P(None, ("kv", "tp")),
        P(None, ("kv", "tp")),
        P(("kv", "tp"), None),
    )
    out_specs = (P(None, ("kv", "tp")), P("kv", "tp", None, None), P("kv", "tp"))
    return jax.shard_map(
        functools.partial(on_device, mesh.shape["kv"], mesh.shape["tp"]),
        mesh=mesh,
        in_specs=in_specs,
        out_specs=out_specs,
        check_vma=False,
    )
```
